32 devices in a mesh: sp: 4 (over y, x), dp: 8 (over z, core).
Axes of the slice: x: 2, y: 2, z: 4, core: 2. Of those that a mesh axis runs over, the one named last changes fastest.
Arguments:
- value_half: bfloat16 [8, 1024, 2048], P('dp', 'sp'), may hold values from -6 to 6
- gate_half: bfloat16 [8, 1024, 2048], P('dp', 'sp'), may hold values from -6 to 6
- upstream: bfloat16 [8, 1024, 2048], P('dp', 'sp'), may hold values from -6 to 6
- conv_taps: float32 [31, 2048], P(None, 'sp'), may hold values from -1 to 1
- norm_gain: float32 [2048], replicated, may hold values from 0.1 to 1.9
- out_weight: bfloat16 [2048, 2048], P('dp'), may hold values from -0.125 to 0.125
Outputs:
- grad_value: bfloat16 [8, 1024, 2048], P('dp', 'sp')
- grad_gate: bfloat16 [8, 1024, 2048], P('dp', 'sp')
- grad_taps: float32 [31, 2048], P(None, 'sp')
- grad_gain: float32 [2048], replicated
- grad_weight: float32 [2048, 2048], P('dp')
The draws below stay inside these ranges and needn't reach their ends.
All inputs are finite; a program needn't handle non-finite values.
Results may differ from the reference program's by a relative error of at most 0.0062.
Values may be sent and summed in bfloat16 or wider, within the bound.
A program may use at most 128 MiB of HBM per device.

```python
import jax
import jax.numpy as jnp
from jax import lax

D = 2048
KERNEL = 31
LENGTH = 1024
BATCH = 8


def spiked(drawn, rng, source, target, parts, factor):
    owner, partner = [(jnp.arange(drawn.shape[dim]) // (drawn.shape[dim] // parts)).reshape([-1 if axis == dim else 1 for axis in range(drawn.ndim)]) for dim in (source, target)]
    chosen = jax.random.permutation(rng, parts)[partner]
    strong = (owner == chosen) | (owner == (partner + parts // 2) % parts)
    return jnp.where(strong, factor * drawn, drawn)


def block_levels(stream_key, dims, pieces, low, largest):
    level = 1.0
    for axis_at, blocks in pieces:
        draws = jax.random.uniform(jax.random.fold_in(jax.random.fold_in(stream_key, 6), axis_at), (blocks,), jnp.float32, low / len(pieces), largest / len(pieces))
        level = level * jnp.repeat(jnp.exp(draws), dims[axis_at] // blocks).reshape((-1,) + (1,) * (len(dims) - 1 - axis_at))
    return level


def normal_values(own_key, shape, scale, bound, pieces=(), held_as=jnp.bfloat16):
    drawn = scale * jax.random.normal(own_key, shape, jnp.float32)
    if pieces:
        drawn = drawn * block_levels(own_key, shape, pieces, -0.22, 0.18)
    return jnp.clip(drawn, -bound, bound).astype(held_as)


def bell_draw_with(rng, shape, spread, limit, cuts, heavy, dtype=jnp.bfloat16):
    drawn = spread * jax.random.normal(rng, shape, jnp.float32)
    if cuts:
        drawn = drawn * block_levels(rng, shape, cuts, -0.22, 0.18)
    return jnp.clip(spiked(drawn, jax.random.fold_in(rng, 3), *heavy), -limit, limit).astype(dtype)


def setup_inputs(seed: int = 0) -> dict:
    splits = jax.random.split(jax.random.key(seed), 7)
    return {
        "value_half": normal_values(splits[0], (BATCH, LENGTH, D), 1.0, 6.0, ((0, 8), (1, 4))),
        "gate_half": normal_values(splits[1], (BATCH, LENGTH, D), 1.0, 6.0, ((0, 8), (1, 4))),
        "upstream": bell_draw_with(splits[2], (BATCH, LENGTH, D), 1.0, 6.0, ((0, 8), (1, 4)), (0, 2, 8, 2.0)),
        "conv_taps": normal_values(splits[3], (KERNEL, D), 0.18, 1.0, ((1, 4),), jnp.float32),
        "norm_gain": jnp.clip(1.0 + 0.18 * jax.random.normal(splits[4], (D,), jnp.float32), 0.1, 1.9),
        "out_weight": normal_values(splits[5], (D, D), D ** -0.5, 0.125, ((0, 8),)),
    }


NORM_EPS = 1e-05

def one_sequence(sequence, conv_taps, norm_gain, out_weight):
    value_half, gate_half, upstream = sequence
    tap_count = conv_taps.shape[0]
    length = value_half.shape[0]
    sig_gate = jax.nn.sigmoid(gate_half.astype(jnp.float32))
    value_wide = value_half.astype(jnp.float32)
    glu = (value_wide * sig_gate).astype(jnp.bfloat16)
    glu_wide = lax.optimization_barrier(glu).astype(jnp.float32)
    padded = jnp.pad(glu_wide, ((tap_count - 1, 0), (0, 0)))
    conv_out = jnp.zeros_like(glu_wide)
    for offset in range(tap_count):
        conv_out = conv_out + conv_taps[offset] * padded[offset:offset + length]
    conv_out = lax.optimization_barrier(conv_out.astype(jnp.bfloat16)).astype(jnp.float32)
    row_mean = lax.optimization_barrier(jnp.mean(conv_out, axis=-1, keepdims=True))
    centered = conv_out - row_mean
    inv_scale = lax.rsqrt(lax.optimization_barrier(jnp.mean(centered * centered, axis=-1, keepdims=True)) + NORM_EPS)
    normed = centered * inv_scale
    scaled = normed * norm_gain
    sig_scaled = jax.nn.sigmoid(scaled)
    activated = (scaled * sig_scaled).astype(jnp.bfloat16)
    grad_act = jnp.dot(upstream, out_weight, preferred_element_type=jnp.float32)
    grad_scaled = grad_act * sig_scaled * (1.0 + scaled * (1.0 - sig_scaled))
    gain_term = lax.optimization_barrier(jnp.sum(grad_scaled * normed, axis=0))
    grad_normed = grad_scaled * norm_gain
    grad_conv_out = inv_scale * (grad_normed - lax.optimization_barrier(jnp.mean(grad_normed, axis=-1, keepdims=True)) - normed * lax.optimization_barrier(jnp.mean(grad_normed * normed, axis=-1, keepdims=True)))
    grad_conv_out = lax.optimization_barrier(grad_conv_out.astype(jnp.bfloat16)).astype(jnp.float32)
    grad_padded = jnp.pad(grad_conv_out, ((0, tap_count - 1), (0, 0)))
    grad_glu = jnp.zeros_like(grad_conv_out)
    tap_terms = []
    for offset in range(tap_count):
        first = tap_count - 1 - offset
        grad_glu = grad_glu + conv_taps[offset] * grad_padded[first:first + length]
        tap_terms.append(lax.optimization_barrier(jnp.sum(grad_conv_out * padded[offset:offset + length], axis=0)))
    grad_glu = lax.optimization_barrier(grad_glu.astype(jnp.bfloat16)).astype(jnp.float32)
    grad_value = (grad_glu * sig_gate).astype(jnp.bfloat16)
    grad_gate = (grad_glu * value_wide * sig_gate * (1.0 - sig_gate)).astype(jnp.bfloat16)
    return (grad_value, grad_gate, activated, jnp.stack(tap_terms), gain_term)

def reference(value_half, gate_half, upstream, conv_taps, norm_gain, out_weight):

    def mapped(sequence):
        return one_sequence(sequence, conv_taps, norm_gain, out_weight)
    grad_value, grad_gate, activated, tap_terms, gain_terms = lax.map(mapped, (value_half, gate_half, upstream))
    model_width = value_half.shape[2]
    grad_weight = lax.dot_general(upstream.reshape(-1, model_width), activated.reshape(-1, model_width), (((0,), (0,)), ((), ())), preferred_element_type=jnp.float32)
    grad_taps = lax.optimization_barrier(jnp.sum(tap_terms, axis=0))
    grad_gain = lax.optimization_barrier(jnp.sum(gain_terms, axis=0))
    return (grad_value, grad_gate, grad_taps, grad_gain, grad_weight)
```

```python
import jax
import jax.numpy as jnp
from jax import lax
from jax.sharding import PartitionSpec as P

NORM_EPS = 1e-05


def body(value_half, gate_half, upstream, conv_taps, norm_gain, out_weight):
    f32 = jnp.float32
    tap_count = conv_taps.shape[0]
    halo = tap_count - 1
    sp = lax.axis_size("sp")
    onward = [(i, i + 1) for i in range(sp - 1)]
    back = [(i + 1, i) for i in range(sp - 1)]

    value = value_half[0].astype(f32)
    gate = gate_half[0].astype(f32)
    length = value.shape[0]
    weight = lax.all_gather(out_weight, "dp", axis=0, tiled=True)
    up = upstream[0]
    up_columns = lax.all_to_all(up, "dp", split_axis=1, concat_axis=0, tiled=True)
    taps = lax.all_gather(conv_taps, "sp", axis=1, tiled=True)

    tail = (value[length - halo :] * jax.nn.sigmoid(gate[length - halo :])).astype(jnp.bfloat16)
    before = lax.ppermute(tail, "sp", onward)
    sig_gate = jax.nn.sigmoid(gate)
    glu = (value * sig_gate).astype(jnp.bfloat16)
    padded = jnp.concatenate([before, glu], axis=0).astype(f32)
    conv = jnp.zeros((length, padded.shape[1]), f32)
    for j in range(tap_count):
        conv = conv + taps[j] * padded[j : j + length]
    conv = conv.astype(jnp.bfloat16).astype(f32)
    mean = jnp.mean(conv, axis=-1, keepdims=True)
    centered = conv - mean
    inv = lax.rsqrt(jnp.mean(centered * centered, axis=-1, keepdims=True) + NORM_EPS)
    normed = centered * inv
    scaled = normed * norm_gain
    sig = jax.nn.sigmoid(scaled)
    activated = (scaled * sig).astype(jnp.bfloat16)
    act_all = lax.all_gather(activated, "dp", axis=0, tiled=True)

    grad_act = jnp.dot(up, weight, preferred_element_type=f32)
    grad_scaled = grad_act * sig * (1.0 + scaled * (1.0 - sig))
    gain_part = jnp.sum(grad_scaled * normed, axis=0)
    g = grad_scaled * norm_gain
    grad_conv = inv * (
        g
        - jnp.mean(g, axis=-1, keepdims=True)
        - normed * jnp.mean(g * normed, axis=-1, keepdims=True)
    )
    grad_conv = grad_conv.astype(jnp.bfloat16)
    after = lax.ppermute(grad_conv[:halo], "sp", back)
    extended = jnp.concatenate([grad_conv, after], axis=0).astype(f32)
    here = grad_conv.astype(f32)
    grad_glu = jnp.zeros_like(here)
    terms = []
    for j in range(tap_count):
        first = halo - j
        grad_glu = grad_glu + taps[j] * extended[first : first + length]
        terms.append(jnp.sum(here * padded[j : j + length], axis=0))
    sums = lax.psum(jnp.stack(terms + [gain_part]), ("sp", "dp"))
    width = conv_taps.shape[1]
    grad_taps = lax.dynamic_slice_in_dim(
        sums[:tap_count], lax.axis_index("sp") * width, width, axis=1
    )
    grad_gain = sums[tap_count]
    grad_glu = grad_glu.astype(jnp.bfloat16).astype(f32)
    grad_value = (grad_glu * sig_gate).astype(jnp.bfloat16)
    grad_gate = (grad_glu * value * sig_gate * (1.0 - sig_gate)).astype(jnp.bfloat16)

    owned = lax.dot_general(
        up_columns, act_all, (((0,), (0,)), ((), ())), preferred_element_type=f32
    )
    grad_weight = lax.psum(owned, "sp")
    return (grad_value[None], grad_gate[None], grad_taps, grad_gain, grad_weight)


def solution(mesh):
    tokens = P("dp", "sp", None)
    return jax.shard_map(
        body,
        mesh=mesh,
        in_specs=(tokens, tokens, tokens, P(None, "sp"), P(), P("dp", None)),
        out_specs=(tokens, tokens, P(None, "sp"), P(), P("dp", None)),
        check_vma=False,
    )
```

```python
import functools

import jax
import jax.numpy as jnp
from jax import lax
from jax.experimental import pallas as pl
from jax.experimental.pallas import tpu as pltpu
from jax.sharding import PartitionSpec as P

NORM_EPS = 1e-05
VMEM = pl.BlockSpec(memory_space=pltpu.VMEM)


class Copies:
    def __init__(self, send, recv, local):
        self.send, self.recv, self.local = send, recv, local
        self.n_remote = self.n_local = 0
        self.remote, self.locals = [], []

    def start(self, src, dst, target):
        i = self.n_remote
        self.n_remote += 1
        copy = pltpu.make_async_remote_copy(
            src_ref=src,
            dst_ref=dst,
            send_sem=self.send.at[i],
            recv_sem=self.recv.at[i],
            device_id=target,
            device_id_type=pl.DeviceIdType.MESH,
        )
        copy.start()
        self.remote.append([copy, False])
        return len(self.remote) - 1

    def keep(self, src, dst):
        copy = pltpu.make_async_copy(src, dst, self.local.at[self.n_local])
        self.n_local += 1
        copy.start()
        self.locals.append(copy)

    def arrive(self, i):
        self.remote[i][0].wait_recv()
        self.remote[i][1] = True

    def finish(self):
        for copy, arrived in self.remote:
            if not arrived:
                copy.wait_recv()
            copy.wait_send()
        for copy in self.locals:
            copy.wait()


def greet(axes):
    barrier = pltpu.get_barrier_semaphore()
    count = 0
    for axis in axes:
        n = lax.axis_size(axis)
        me = lax.axis_index(axis)
        for k in range(1, n):
            pl.semaphore_signal(
                barrier,
                inc=1,
                device_id={axis: lax.rem(me + k, n)},
                device_id_type=pl.DeviceIdType.MESH,
            )
            count += 1
    pl.semaphore_wait(barrier, count)


def direct(copies, kind, axis, src, dst):
    n = lax.axis_size(axis)
    me = lax.axis_index(axis)
    if kind == "next" or kind == "prev":
        copies.start(src, dst, {axis: lax.rem(me + (1 if kind == "next" else n - 1), n)})
        return
    copies.keep(src.at[me] if kind == "scatter" else src, dst.at[me])
    for k in range(1, n):
        peer = lax.rem(me + k, n)
        copies.start(src.at[peer] if kind == "scatter" else src, dst.at[me], {axis: peer})


def spread_gather(copies, src, dst):
    ns, nz = lax.axis_size("sp"), lax.axis_size("dp") // 2
    s, d = lax.axis_index("sp"), lax.axis_index("dp")
    z, c = d // 2, lax.rem(d, 2)
    partner = {"dp": d + 1 - 2 * c}
    first = [
        copies.start(src.at[s], dst.at[d, s], {"dp": 2 * lax.rem(z + k, nz) + c})
        for k in range(1, nz)
    ]
    copies.keep(src, dst.at[d])
    copies.start(src, dst.at[d], partner)
    second = {}
    for k in range(1, nz):
        copies.arrive(first[k - 1])
        piece = dst.at[2 * lax.rem(z + nz - k, nz) + c, s]
        for j in range(1, ns):
            second[k, j] = copies.start(piece, piece, {"sp": lax.rem(s + j, ns)})
        copies.start(piece, piece, partner)
    for k in range(1, nz):
        for j in range(1, ns):
            copies.arrive(second[k, j])
            piece = dst.at[2 * lax.rem(z + nz - k, nz) + c, lax.rem(s + ns - j, ns)]
            copies.start(piece, piece, partner)


def ring_gather(copies, src, dst):
    nz = lax.axis_size("dp") // 2
    d = lax.axis_index("dp")
    z, c = d // 2, lax.rem(d, 2)
    partner = {"dp": d + 1 - 2 * c}
    up = {"dp": 2 * lax.rem(z + 1, nz) + c}
    down = {"dp": 2 * lax.rem(z + nz - 1, nz) + c}
    a = copies.start(src.at[0], dst.at[d, 0], up)
    b = copies.start(src.at[1], dst.at[d, 1], down)
    copies.keep(src, dst.at[d])
    copies.start(src, dst.at[d], partner)
    for k in range(1, nz):
        low = dst.at[2 * lax.rem(z + nz - k, nz) + c, 0]
        high = dst.at[2 * lax.rem(z + k, nz) + c, 1]
        copies.arrive(a)
        if k < nz - 1:
            a = copies.start(low, low, up)
        copies.arrive(b)
        if k < nz - 1:
            b = copies.start(high, high, down)
        copies.start(low, low, partner)
        copies.start(high, high, partner)


def run(axes, items, *refs):
    n = len(items)
    copies = Copies(*refs[2 * n :])
    greet(axes)
    for i, (kind, axis) in enumerate(items):
        src, dst = refs[i], refs[n + i]
        if kind == "spread":
            spread_gather(copies, src, dst)
        elif kind == "ring":
            ring_gather(copies, src, dst)
        else:
            direct(copies, kind, axis, src, dst)
    copies.finish()


def exchange(collective_id, *items):
    ns, nd = lax.axis_size("sp"), lax.axis_size("dp")
    shapes, remote, local = [], 0, 0
    for kind, axis, x in items:
        n = lax.axis_size(axis)
        if kind in ("next", "prev"):
            shape = x.shape
            remote += 1
        elif kind == "scatter":
            shape = x.shape
            remote += n - 1
            local += 1
        else:
            shape = (n,) + x.shape
            local += 1
            if kind == "gather":
                remote += n - 1
            elif kind == "spread":
                remote += (nd // 2 - 1) * 2 * ns + 1
            else:
                remote += (nd // 2 - 1) * 4 + 1
        shapes.append(jax.ShapeDtypeStruct(shape, x.dtype))
    axes = tuple(a for a in ("sp", "dp") if any(axis == a or kind == "spread" for kind, axis, _ in items))
    return pl.pallas_call(
        functools.partial(run, axes, tuple((kind, axis) for kind, axis, _ in items)),
        out_shape=shapes,
        in_specs=[VMEM] * len(items),
        out_specs=[VMEM] * len(items),
        scratch_shapes=[
            pltpu.SemaphoreType.DMA((remote,)),
            pltpu.SemaphoreType.DMA((remote,)),
            pltpu.SemaphoreType.DMA((max(local, 1),)),
        ],
        compiler_params=pltpu.CompilerParams(
            collective_id=collective_id, has_side_effects=True, vmem_limit_bytes=48 * 1024 * 1024
        ),
    )(*[x for _, _, x in items])


def body(value_half, gate_half, upstream, conv_taps, norm_gain, out_weight):
    f32 = jnp.float32
    tap_count = conv_taps.shape[0]
    halo = tap_count - 1
    nsp, ndp = lax.axis_size("sp"), lax.axis_size("dp")
    at_start = lax.axis_index("sp") == 0
    at_end = lax.axis_index("sp") == nsp - 1
    edge = (halo + 15) // 16 * 16

    value = value_half[0].astype(f32)
    gate = gate_half[0].astype(f32)
    length = value.shape[0]
    channels = value.shape[1]
    up = upstream[0]
    rows = out_weight.shape[0]

    tail = (value[length - edge :] * jax.nn.sigmoid(gate[length - edge :])).astype(jnp.bfloat16)
    up_blocks = jnp.swapaxes(up.reshape(length, ndp, rows), 0, 1)
    before, taps, up_columns, weight = exchange(
        1,
        ("next", "sp", tail),
        ("gather", "sp", conv_taps),
        ("scatter", "dp", up_blocks),
        ("spread", "dp", out_weight.reshape(nsp, rows // nsp, channels)),
    )
    before = jnp.where(at_start, 0, before)[edge - halo :]
    taps = jnp.swapaxes(taps, 0, 1).reshape(tap_count, channels)
    up_columns = up_columns.reshape(ndp * length, rows)
    weight = weight.reshape(ndp * rows, channels)
    sig_gate = jax.nn.sigmoid(gate)
    glu = (value * sig_gate).astype(jnp.bfloat16)
    padded = jnp.concatenate([before, glu], axis=0).astype(f32)
    conv = jnp.zeros((length, padded.shape[1]), f32)
    for j in range(tap_count):
        conv = conv + taps[j] * padded[j : j + length]
    conv = conv.astype(jnp.bfloat16).astype(f32)
    mean = jnp.mean(conv, axis=-1, keepdims=True)
    centered = conv - mean
    inv = lax.rsqrt(jnp.mean(centered * centered, axis=-1, keepdims=True) + NORM_EPS)
    normed = centered * inv
    scaled = normed * norm_gain
    sig = jax.nn.sigmoid(scaled)
    activated = (scaled * sig).astype(jnp.bfloat16)

    grad_act = jnp.dot(up, weight, preferred_element_type=f32)
    grad_scaled = grad_act * sig * (1.0 + scaled * (1.0 - sig))
    gain_part = jnp.sum(grad_scaled * normed, axis=0)
    g = grad_scaled * norm_gain
    grad_conv = inv * (
        g
        - jnp.mean(g, axis=-1, keepdims=True)
        - normed * jnp.mean(g * normed, axis=-1, keepdims=True)
    )
    grad_conv = grad_conv.astype(jnp.bfloat16)
    after, act_all = exchange(
        2,
        ("prev", "sp", grad_conv[:edge]),
        ("ring", "dp", activated.reshape(2, length // 2, channels)),
    )
    after = jnp.where(at_end, 0, after)[:halo]
    act_all = act_all.reshape(ndp * length, channels)
    extended = jnp.concatenate([grad_conv, after], axis=0).astype(f32)
    here = grad_conv.astype(f32)
    grad_glu = jnp.zeros_like(here)
    terms = []
    for j in range(tap_count):
        first = halo - j
        grad_glu = grad_glu + taps[j] * extended[first : first + length]
        terms.append(jnp.sum(here * padded[j : j + length], axis=0))
    grad_glu = grad_glu.astype(jnp.bfloat16).astype(f32)
    grad_value = (grad_glu * sig_gate).astype(jnp.bfloat16)
    grad_gate = (grad_glu * value * sig_gate * (1.0 - sig_gate)).astype(jnp.bfloat16)

    owned = lax.dot_general(
        up_columns, act_all, (((0,), (0,)), ((), ())), preferred_element_type=f32
    )
    width = conv_taps.shape[1]
    tap_blocks = jnp.swapaxes(jnp.stack(terms).reshape(tap_count, nsp, width), 0, 1)
    gain_got, tap_got, owned_got = exchange(
        3,
        ("gather", "sp", gain_part[None]),
        ("scatter", "sp", tap_blocks),
        ("scatter", "sp", owned.astype(jnp.bfloat16).reshape(nsp, rows // nsp, channels)),
    )
    gain_got, tap_got, grad_weight = exchange(
        4,
        ("gather", "dp", jnp.sum(gain_got, axis=0)),
        ("gather", "dp", jnp.sum(tap_got, axis=0)),
        ("gather", "sp", jnp.sum(owned_got.astype(f32), axis=0).astype(jnp.bfloat16)),
    )
    grad_gain = jnp.sum(gain_got, axis=0)[0]
    grad_taps = jnp.sum(tap_got, axis=0)
    grad_weight = grad_weight.reshape(rows, channels).astype(f32)
    return (grad_value[None], grad_gate[None], grad_taps, grad_gain, grad_weight)


def solution(mesh):
    tokens = P("dp", "sp", None)
    return jax.shard_map(
        body,
        mesh=mesh,
        in_specs=(tokens, tokens, tokens, P(None, "sp"), P(), P("dp", None)),
        out_specs=(tokens, tokens, P(None, "sp"), P(), P("dp", None)),
        check_vma=False,
    )
```

```python
import functools

import jax
import jax.numpy as jnp
from jax import lax
from jax.experimental import pallas as pl
from jax.experimental.pallas import tpu as pltpu
from jax.sharding import PartitionSpec as P

NORM_EPS = 1e-05
VMEM = pl.BlockSpec(memory_space=pltpu.VMEM)


def when(condition, act):
    if condition is None:
        act()
    else:
        pl.when(condition)(lambda: act())


class Copies:
    def __init__(self, send, recv, local):
        self.send, self.recv, self.local = send, recv, local
        self.n_remote = self.n_local = 0
        self.remote, self.locals = [], []

    def start(self, src, dst, target, sends=None, receives=None):
        i = self.n_remote
        self.n_remote += 1
        copy = pltpu.make_async_remote_copy(
            src_ref=src,
            dst_ref=dst,
            send_sem=self.send.at[i],
            recv_sem=self.recv.at[i],
            device_id=target,
            device_id_type=pl.DeviceIdType.MESH,
        )
        when(sends, copy.start)
        self.remote.append([copy, False, sends, receives])
        return len(self.remote) - 1

    def keep(self, src, dst):
        copy = pltpu.make_async_copy(src, dst, self.local.at[self.n_local])
        self.n_local += 1
        copy.start()
        self.locals.append(copy)

    def arrive(self, i):
        when(self.remote[i][3], self.remote[i][0].wait_recv)
        self.remote[i][1] = True

    def finish(self):
        for copy, arrived, sends, receives in self.remote:
            if not arrived:
                when(receives, copy.wait_recv)
            when(sends, copy.wait_send)
        for copy in self.locals:
            copy.wait()


def greet(axes):
    barrier = pltpu.get_barrier_semaphore()
    count = 0
    for axis in axes:
        n = lax.axis_size(axis)
        me = lax.axis_index(axis)
        for k in range(1, n):
            pl.semaphore_signal(
                barrier,
                inc=1,
                device_id={axis: lax.rem(me + k, n)},
                device_id_type=pl.DeviceIdType.MESH,
            )
            count += 1
    pl.semaphore_wait(barrier, count)


def direct(copies, kind, axis, src, dst):
    n = lax.axis_size(axis)
    me = lax.axis_index(axis)
    if kind == "next" or kind == "prev":
        copies.start(src, dst, {axis: lax.rem(me + (1 if kind == "next" else n - 1), n)})
        return
    copies.keep(src.at[me] if kind == "scatter" else src, dst.at[me])
    for k in range(1, n):
        peer = lax.rem(me + k, n)
        copies.start(src.at[peer] if kind == "scatter" else src, dst.at[me], {axis: peer})


def spread_gather(copies, src, dst):
    ns, nz = lax.axis_size("sp"), lax.axis_size("dp") // 2
    s, d = lax.axis_index("sp"), lax.axis_index("dp")
    z, c = d // 2, lax.rem(d, 2)
    partner = {"dp": d + 1 - 2 * c}
    first = [
        copies.start(src.at[s], dst.at[d, s], {"dp": 2 * lax.rem(z + k, nz) + c})
        for k in range(1, nz)
    ]
    yield
    copies.keep(src, dst.at[d])
    copies.start(src, dst.at[d], partner)
    second = {}
    for k in range(1, nz):
        copies.arrive(first[k - 1])
        piece = dst.at[2 * lax.rem(z + nz - k, nz) + c, s]
        for j in range(1, ns):
            second[k, j] = copies.start(piece, piece, {"sp": lax.rem(s + j, ns)})
        copies.start(piece, piece, partner)
    yield
    for k in range(1, nz):
        for j in range(1, ns):
            copies.arrive(second[k, j])
            piece = dst.at[2 * lax.rem(z + nz - k, nz) + c, lax.rem(s + ns - j, ns)]
            copies.start(piece, piece, partner)


def line_gather(copies, src, dst):
    nz = lax.axis_size("dp") // 2
    d = lax.axis_index("dp")
    z, c = d // 2, lax.rem(d, 2)
    partner = {"dp": d + 1 - 2 * c}
    up = {"dp": 2 * lax.rem(z + 1, nz) + c}
    down = {"dp": 2 * lax.rem(z + nz - 1, nz) + c}
    below, above = {}, {}

    def send(k):
        low, high = 2 * lax.rem(z + nz - k, nz) + c, 2 * lax.rem(z + k, nz) + c
        low_src, high_src = (dst.at[low], dst.at[high]) if k else (src, src)
        below[k] = copies.start(
            low_src, dst.at[low], up, jnp.logical_and(z >= k, z < nz - 1), z >= k + 1
        )
        above[k] = copies.start(
            high_src, dst.at[high], down, jnp.logical_and(z + k < nz, z > 0), z + k + 1 < nz
        )

    send(0)
    yield
    copies.keep(src, dst.at[d])
    copies.start(src, dst.at[d], partner)
    for k in range(1, nz):
        copies.arrive(below[k - 1])
        copies.arrive(above[k - 1])
        if k < nz - 1:
            send(k)
        low, high = dst.at[2 * lax.rem(z + nz - k, nz) + c], dst.at[2 * lax.rem(z + k, nz) + c]
        copies.start(low, low, partner, z >= k, z >= k)
        copies.start(high, high, partner, z + k < nz, z + k < nz)
        yield


def run(axes, items, *refs):
    n = len(items)
    copies = Copies(*refs[2 * n :])
    greet(axes)
    waiting = []
    for i, (kind, axis) in enumerate(items):
        src, dst = refs[i], refs[n + i]
        if kind == "spread":
            waiting.append(spread_gather(copies, src, dst))
        elif kind == "line":
            waiting.append(line_gather(copies, src, dst))
        elif kind == "later":
            waiting.append(later(copies, axis, src, dst))
        else:
            direct(copies, kind, axis, src, dst)
    while waiting:
        waiting = [steps for steps in waiting if next(steps, waiting) is None]
    copies.finish()


def later(copies, axis, src, dst):
    yield
    direct(copies, "scatter", axis, src, dst)


def exchange(collective_id, *items):
    ns, nd = lax.axis_size("sp"), lax.axis_size("dp")
    shapes, remote, local = [], 0, 0
    for kind, axis, x in items:
        n = lax.axis_size(axis)
        if kind in ("next", "prev"):
            shape = x.shape
            remote += 1
        elif kind in ("scatter", "later"):
            shape = x.shape
            remote += n - 1
            local += 1
        else:
            shape = (n,) + x.shape
            local += 1
            if kind == "gather":
                remote += n - 1
            elif kind == "spread":
                remote += (nd // 2 - 1) * 2 * ns + 1
            else:
                remote += (nd // 2 - 1) * 4 + 1
        shapes.append(jax.ShapeDtypeStruct(shape, x.dtype))
    axes = tuple(a for a in ("sp", "dp") if any(axis == a or kind == "spread" for kind, axis, _ in items))
    return pl.pallas_call(
        functools.partial(run, axes, tuple((kind, axis) for kind, axis, _ in items)),
        out_shape=shapes,
        in_specs=[VMEM] * len(items),
        out_specs=[VMEM] * len(items),
        scratch_shapes=[
            pltpu.SemaphoreType.DMA((remote,)),
            pltpu.SemaphoreType.DMA((remote,)),
            pltpu.SemaphoreType.DMA((max(local, 1),)),
        ],
        compiler_params=pltpu.CompilerParams(
            collective_id=collective_id, has_side_effects=True, vmem_limit_bytes=48 * 1024 * 1024
        ),
    )(*[x for _, _, x in items])


def body(value_half, gate_half, upstream, conv_taps, norm_gain, out_weight):
    f32 = jnp.float32
    tap_count = conv_taps.shape[0]
    halo = tap_count - 1
    nsp, ndp = lax.axis_size("sp"), lax.axis_size("dp")
    at_start = lax.axis_index("sp") == 0
    at_end = lax.axis_index("sp") == nsp - 1
    edge = (halo + 15) // 16 * 16

    value = value_half[0].astype(f32)
    gate = gate_half[0].astype(f32)
    length = value.shape[0]
    channels = value.shape[1]
    up = upstream[0]
    rows = out_weight.shape[0]

    tail = (value[length - edge :] * jax.nn.sigmoid(gate[length - edge :])).astype(jnp.bfloat16)
    up_blocks = jnp.swapaxes(up.reshape(length, ndp, rows), 0, 1)
    before, taps = exchange(1, ("next", "sp", tail), ("gather", "sp", conv_taps))
    before = jnp.where(at_start, 0, before)[edge - halo :]
    taps = jnp.swapaxes(taps, 0, 1).reshape(tap_count, channels)
    sig_gate = jax.nn.sigmoid(gate)
    glu = (value * sig_gate).astype(jnp.bfloat16)
    padded = jnp.concatenate([before, glu], axis=0).astype(f32)
    conv = jnp.zeros((length, padded.shape[1]), f32)
    for j in range(tap_count):
        conv = conv + taps[j] * padded[j : j + length]
    conv = conv.astype(jnp.bfloat16).astype(f32)
    mean = jnp.mean(conv, axis=-1, keepdims=True)
    centered = conv - mean
    inv = lax.rsqrt(jnp.mean(centered * centered, axis=-1, keepdims=True) + NORM_EPS)
    normed = centered * inv
    scaled = normed * norm_gain
    sig = jax.nn.sigmoid(scaled)
    activated = (scaled * sig).astype(jnp.bfloat16)

    weight, act_all, up_columns = exchange(
        2,
        ("spread", "dp", out_weight.reshape(nsp, rows // nsp, channels)),
        ("line", "dp", activated),
        ("later", "dp", up_blocks),
    )
    weight = weight.reshape(ndp * rows, channels)
    act_all = act_all.reshape(ndp * length, channels)
    up_columns = up_columns.reshape(ndp * length, rows)
    owned = lax.dot_general(
        up_columns, act_all, (((0,), (0,)), ((), ())), preferred_element_type=f32
    )

    grad_act = jnp.dot(up, weight, preferred_element_type=f32)
    grad_scaled = grad_act * sig * (1.0 + scaled * (1.0 - sig))
    gain_part = jnp.sum(grad_scaled * normed, axis=0)
    g = grad_scaled * norm_gain
    grad_conv = inv * (
        g
        - jnp.mean(g, axis=-1, keepdims=True)
        - normed * jnp.mean(g * normed, axis=-1, keepdims=True)
    )
    grad_conv = grad_conv.astype(jnp.bfloat16)
    after, gain_got, owned_got = exchange(
        3,
        ("prev", "sp", grad_conv[:edge]),
        ("gather", "sp", gain_part[None]),
        ("scatter", "sp", owned.astype(jnp.bfloat16).reshape(nsp, rows // nsp, channels)),
    )
    after = jnp.where(at_end, 0, after)[:halo]
    extended = jnp.concatenate([grad_conv, after], axis=0).astype(f32)
    here = grad_conv.astype(f32)
    grad_glu = jnp.zeros_like(here)
    terms = []
    for j in range(tap_count):
        first = halo - j
        grad_glu = grad_glu + taps[j] * extended[first : first + length]
        terms.append(jnp.sum(here * padded[j : j + length], axis=0))
    grad_glu = grad_glu.astype(jnp.bfloat16).astype(f32)
    grad_value = (grad_glu * sig_gate).astype(jnp.bfloat16)
    grad_gate = (grad_glu * value * sig_gate * (1.0 - sig_gate)).astype(jnp.bfloat16)

    width = conv_taps.shape[1]
    tap_blocks = jnp.swapaxes(jnp.stack(terms).reshape(tap_count, nsp, width), 0, 1)
    gain_got, tap_got, grad_weight = exchange(
        4,
        ("gather", "dp", jnp.sum(gain_got, axis=0)),
        ("scatter", "sp", tap_blocks),
        ("gather", "sp", jnp.sum(owned_got.astype(f32), axis=0).astype(jnp.bfloat16)),
    )
    (tap_got,) = exchange(5, ("gather", "dp", jnp.sum(tap_got, axis=0)))
    grad_gain = jnp.sum(gain_got, axis=0)[0]
    grad_taps = jnp.sum(tap_got, axis=0)
    grad_weight = grad_weight.reshape(rows, channels).astype(f32)
    return (grad_value[None], grad_gate[None], grad_taps, grad_gain, grad_weight)


def solution(mesh):
    tokens = P("dp", "sp", None)
    return jax.shard_map(
        body,
        mesh=mesh,
        in_specs=(tokens, tokens, tokens, P(None, "sp"), P(), P("dp", None)),
        out_specs=(tokens, tokens, P(None, "sp"), P(), P("dp", None)),
        check_vma=False,
    )
```

```python
import functools

import jax
import jax.numpy as jnp
from jax import lax
from jax.experimental import pallas as pl
from jax.experimental.pallas import tpu as pltpu
from jax.sharding import PartitionSpec as P

NORM_EPS = 1e-05
VMEM = pl.BlockSpec(memory_space=pltpu.VMEM)


def when(condition, act):
    if condition is None:
        act()
    else:
        pl.when(condition)(lambda: act())


class Copies:
    def __init__(self, send, recv, local):
        self.send, self.recv, self.local = send, recv, local
        self.n_remote = self.n_local = 0
        self.remote, self.locals = [], []

    def start(self, src, dst, target, sends=None, receives=None):
        i = self.n_remote
        self.n_remote += 1
        copy = pltpu.make_async_remote_copy(
            src_ref=src,
            dst_ref=dst,
            send_sem=self.send.at[i],
            recv_sem=self.recv.at[i],
            device_id=target,
            device_id_type=pl.DeviceIdType.MESH,
        )
        when(sends, copy.start)
        self.remote.append([copy, False, sends, receives])
        return len(self.remote) - 1

    def keep(self, src, dst):
        copy = pltpu.make_async_copy(src, dst, self.local.at[self.n_local])
        self.n_local += 1
        copy.start()
        self.locals.append(copy)

    def arrive(self, i):
        when(self.remote[i][3], self.remote[i][0].wait_recv)
        self.remote[i][1] = True

    def finish(self):
        for copy, arrived, sends, receives in self.remote:
            if not arrived:
                when(receives, copy.wait_recv)
            when(sends, copy.wait_send)
        for copy in self.locals:
            copy.wait()


def greet(axes):
    barrier = pltpu.get_barrier_semaphore()
    count = 0
    for axis in axes:
        n = lax.axis_size(axis)
        me = lax.axis_index(axis)
        for k in range(1, n):
            pl.semaphore_signal(
                barrier,
                inc=1,
                device_id={axis: lax.rem(me + k, n)},
                device_id_type=pl.DeviceIdType.MESH,
            )
            count += 1
    pl.semaphore_wait(barrier, count)


def direct(copies, kind, axis, src, dst):
    n = lax.axis_size(axis)
    me = lax.axis_index(axis)
    if kind == "next" or kind == "prev":
        copies.start(src, dst, {axis: lax.rem(me + (1 if kind == "next" else n - 1), n)})
        return
    if kind == "pair":
        copies.start(src, dst, {axis: me + 1 - 2 * lax.rem(me, 2)})
        return
    if kind == "rows":
        nz, z, c = n // 2, me // 2, lax.rem(me, 2)
        copies.keep(src.at[z], dst.at[z])
        for k in range(1, nz):
            peer = lax.rem(z + k, nz)
            copies.start(src.at[peer], dst.at[z], {axis: 2 * peer + c})
        return
    copies.keep(src.at[me] if kind == "scatter" else src, dst.at[me])
    for k in range(1, n):
        peer = lax.rem(me + k, n)
        copies.start(src.at[peer] if kind == "scatter" else src, dst.at[me], {axis: peer})


def spread_gather(copies, src, dst):
    ns, nz = lax.axis_size("sp"), lax.axis_size("dp") // 2
    s, d = lax.axis_index("sp"), lax.axis_index("dp")
    z, c = d // 2, lax.rem(d, 2)
    partner = {"dp": d + 1 - 2 * c}
    first = [
        copies.start(src.at[s], dst.at[d, s], {"dp": 2 * lax.rem(z + k, nz) + c})
        for k in range(1, nz)
    ]
    yield
    copies.keep(src, dst.at[d])
    copies.start(src, dst.at[d], partner)
    second = {}
    for k in range(1, nz):
        copies.arrive(first[k - 1])
        piece = dst.at[2 * lax.rem(z + nz - k, nz) + c, s]
        for j in range(1, ns):
            second[k, j] = copies.start(piece, piece, {"sp": lax.rem(s + j, ns)})
        copies.start(piece, piece, partner)
    yield
    for k in range(1, nz):
        for j in range(1, ns):
            copies.arrive(second[k, j])
            piece = dst.at[2 * lax.rem(z + nz - k, nz) + c, lax.rem(s + ns - j, ns)]
            copies.start(piece, piece, partner)


def line_gather(copies, src, dst):
    nz = lax.axis_size("dp") // 2
    d = lax.axis_index("dp")
    z, c = d // 2, lax.rem(d, 2)
    partner = {"dp": d + 1 - 2 * c}
    up = {"dp": 2 * lax.rem(z + 1, nz) + c}
    down = {"dp": 2 * lax.rem(z + nz - 1, nz) + c}
    below, above = {}, {}

    def send(k):
        low, high = 2 * lax.rem(z + nz - k, nz) + c, 2 * lax.rem(z + k, nz) + c
        low_src, high_src = (dst.at[low], dst.at[high]) if k else (src, src)
        below[k] = copies.start(
            low_src, dst.at[low], up, jnp.logical_and(z >= k, z < nz - 1), z >= k + 1
        )
        above[k] = copies.start(
            high_src, dst.at[high], down, jnp.logical_and(z + k < nz, z > 0), z + k + 1 < nz
        )

    send(0)
    yield
    copies.keep(src, dst.at[d])
    copies.start(src, dst.at[d], partner)
    for k in range(1, nz):
        copies.arrive(below[k - 1])
        copies.arrive(above[k - 1])
        if k < nz - 1:
            send(k)
        low, high = dst.at[2 * lax.rem(z + nz - k, nz) + c], dst.at[2 * lax.rem(z + k, nz) + c]
        copies.start(low, low, partner, z >= k, z >= k)
        copies.start(high, high, partner, z + k < nz, z + k < nz)
        yield


def run(axes, items, *refs):
    n = len(items)
    copies = Copies(*refs[2 * n :])
    greet(axes)
    waiting = []
    for i, (kind, axis) in enumerate(items):
        src, dst = refs[i], refs[n + i]
        if kind == "spread":
            waiting.append(spread_gather(copies, src, dst))
        elif kind == "line":
            waiting.append(line_gather(copies, src, dst))
        elif kind == "later":
            waiting.append(later(copies, axis, src, dst))
        else:
            direct(copies, kind, axis, src, dst)
    while waiting:
        waiting = [steps for steps in waiting if next(steps, waiting) is None]
    copies.finish()


def later(copies, axis, src, dst):
    yield
    direct(copies, "scatter", axis, src, dst)


def exchange(collective_id, *items):
    ns, nd = lax.axis_size("sp"), lax.axis_size("dp")
    shapes, remote, local = [], 0, 0
    for kind, axis, x in items:
        n = lax.axis_size(axis)
        if kind == "rows":
            shape = x.shape
            remote += n // 2 - 1
            local += 1
        elif kind in ("next", "prev", "pair"):
            shape = x.shape
            remote += 1
        elif kind in ("scatter", "later"):
            shape = x.shape
            remote += n - 1
            local += 1
        else:
            shape = (n,) + x.shape
            local += 1
            if kind == "gather":
                remote += n - 1
            elif kind == "spread":
                remote += (nd // 2 - 1) * 2 * ns + 1
            else:
                remote += (nd // 2 - 1) * 4 + 1
        shapes.append(jax.ShapeDtypeStruct(shape, x.dtype))
    axes = tuple(a for a in ("sp", "dp") if any(axis == a or kind == "spread" for kind, axis, _ in items))
    return pl.pallas_call(
        functools.partial(run, axes, tuple((kind, axis) for kind, axis, _ in items)),
        out_shape=shapes,
        in_specs=[VMEM] * len(items),
        out_specs=[VMEM] * len(items),
        scratch_shapes=[
            pltpu.SemaphoreType.DMA((remote,)),
            pltpu.SemaphoreType.DMA((remote,)),
            pltpu.SemaphoreType.DMA((max(local, 1),)),
        ],
        compiler_params=pltpu.CompilerParams(
            collective_id=collective_id, has_side_effects=True, vmem_limit_bytes=48 * 1024 * 1024
        ),
    )(*[x for _, _, x in items])


def body(value_half, gate_half, upstream, conv_taps, norm_gain, out_weight):
    f32 = jnp.float32
    tap_count = conv_taps.shape[0]
    halo = tap_count - 1
    nsp, ndp = lax.axis_size("sp"), lax.axis_size("dp")
    at_start = lax.axis_index("sp") == 0
    at_end = lax.axis_index("sp") == nsp - 1
    edge = (halo + 15) // 16 * 16

    value = value_half[0].astype(f32)
    gate = gate_half[0].astype(f32)
    length = value.shape[0]
    channels = value.shape[1]
    up = upstream[0]
    rows = out_weight.shape[0]

    tail = (value[length - edge :] * jax.nn.sigmoid(gate[length - edge :])).astype(jnp.bfloat16)
    up_blocks = jnp.swapaxes(up.reshape(length, ndp, rows), 0, 1)
    before, taps = exchange(1, ("next", "sp", tail), ("gather", "sp", conv_taps))
    before = jnp.where(at_start, 0, before)[edge - halo :]
    taps = jnp.swapaxes(taps, 0, 1).reshape(tap_count, channels)
    sig_gate = jax.nn.sigmoid(gate)
    glu = (value * sig_gate).astype(jnp.bfloat16)
    padded = jnp.concatenate([before, glu], axis=0).astype(f32)
    conv = jnp.zeros((length, padded.shape[1]), f32)
    for j in range(tap_count):
        conv = conv + taps[j] * padded[j : j + length]
    conv = conv.astype(jnp.bfloat16).astype(f32)
    mean = jnp.mean(conv, axis=-1, keepdims=True)
    centered = conv - mean
    inv = lax.rsqrt(jnp.mean(centered * centered, axis=-1, keepdims=True) + NORM_EPS)
    normed = centered * inv
    scaled = normed * norm_gain
    sig = jax.nn.sigmoid(scaled)
    activated = (scaled * sig).astype(jnp.bfloat16)

    half = channels // 2
    nz, piece = ndp // 2, rows // nsp
    core = lax.rem(lax.axis_index("dp"), 2)
    by_core = up.reshape(length, nz, 2, nsp, piece)

    def partial(which):
        columns = lax.dynamic_index_in_dim(by_core, which, 2, keepdims=False)
        columns = jnp.swapaxes(columns, 1, 2).reshape(length, nsp * nz * piece)
        return lax.dot_general(
            columns, activated[:, half:], (((0,), (0,)), ((), ())), preferred_element_type=f32
        )

    weight, act_all, up_columns, from_partner = exchange(
        2,
        ("spread", "dp", out_weight.reshape(nsp, rows // nsp, channels)),
        ("line", "dp", activated[:, :half]),
        ("later", "dp", up_blocks),
        ("pair", "dp", partial(1 - core).astype(jnp.bfloat16)),
    )
    weight = weight.reshape(ndp * rows, channels)
    act_all = act_all.reshape(ndp * length, half)
    up_columns = up_columns.reshape(ndp * length, rows)
    owned = lax.dot_general(
        up_columns, act_all, (((0,), (0,)), ((), ())), preferred_element_type=f32
    )
    summed = (partial(core) + from_partner.astype(f32)).astype(jnp.bfloat16)
    summed = summed.reshape(nsp, nz, piece, half)

    grad_act = jnp.dot(up, weight, preferred_element_type=f32)
    grad_scaled = grad_act * sig * (1.0 + scaled * (1.0 - sig))
    gain_part = jnp.sum(grad_scaled * normed, axis=0)
    g = grad_scaled * norm_gain
    grad_conv = inv * (
        g
        - jnp.mean(g, axis=-1, keepdims=True)
        - normed * jnp.mean(g * normed, axis=-1, keepdims=True)
    )
    grad_conv = grad_conv.astype(jnp.bfloat16)
    after, gain_got, owned_got, summed_got = exchange(
        3,
        ("prev", "sp", grad_conv[:edge]),
        ("gather", "sp", gain_part[None]),
        ("scatter", "sp", owned.astype(jnp.bfloat16).reshape(nsp, piece, half)),
        ("scatter", "sp", summed),
    )
    after = jnp.where(at_end, 0, after)[:halo]
    extended = jnp.concatenate([grad_conv, after], axis=0).astype(f32)
    here = grad_conv.astype(f32)
    grad_glu = jnp.zeros_like(here)
    terms = []
    for j in range(tap_count):
        first = halo - j
        grad_glu = grad_glu + taps[j] * extended[first : first + length]
        terms.append(jnp.sum(here * padded[j : j + length], axis=0))
    grad_glu = grad_glu.astype(jnp.bfloat16).astype(f32)
    grad_value = (grad_glu * sig_gate).astype(jnp.bfloat16)
    grad_gate = (grad_glu * value * sig_gate * (1.0 - sig_gate)).astype(jnp.bfloat16)

    width = conv_taps.shape[1]
    tap_blocks = jnp.swapaxes(jnp.stack(terms).reshape(tap_count, nsp, width), 0, 1)
    gain_got, tap_got, low_weight, high_got = exchange(
        4,
        ("gather", "dp", jnp.sum(gain_got, axis=0)),
        ("scatter", "sp", tap_blocks),
        ("gather", "sp", jnp.sum(owned_got.astype(f32), axis=0).astype(jnp.bfloat16)),
        ("rows", "dp", jnp.sum(summed_got.astype(f32), axis=0).astype(jnp.bfloat16)),
    )
    tap_got, high_weight = exchange(
        5,
        ("gather", "dp", jnp.sum(tap_got, axis=0)),
        ("gather", "sp", jnp.sum(high_got.astype(f32), axis=0).astype(jnp.bfloat16)),
    )
    grad_gain = jnp.sum(gain_got, axis=0)[0]
    grad_taps = jnp.sum(tap_got, axis=0)
    grad_weight = jnp.concatenate(
        [low_weight.reshape(rows, half), high_weight.reshape(rows, half)], axis=1
    ).astype(f32)
    return (grad_value[None], grad_gate[None], grad_taps, grad_gain, grad_weight)


def solution(mesh):
    tokens = P("dp", "sp", None)
    return jax.shard_map(
        body,
        mesh=mesh,
        in_specs=(tokens, tokens, tokens, P(None, "sp"), P(), P("dp", None)),
        out_specs=(tokens, tokens, P(None, "sp"), P(), P("dp", None)),
        check_vma=False,
    )
```

```python
import functools

import jax
import jax.numpy as jnp
from jax import lax
from jax.experimental import pallas as pl
from jax.experimental.pallas import tpu as pltpu
from jax.sharding import PartitionSpec as P

NORM_EPS = 1e-05
VMEM = pl.BlockSpec(memory_space=pltpu.VMEM)


def when(condition, act):
    if condition is None:
        act()
    else:
        pl.when(condition)(lambda: act())


class Copies:
    def __init__(self, send, recv, local):
        self.send, self.recv, self.local = send, recv, local
        self.n_remote = self.n_local = 0
        self.remote, self.locals = [], []

    def start(self, src, dst, target, sends=None, receives=None):
        i = self.n_remote
        self.n_remote += 1
        copy = pltpu.make_async_remote_copy(
            src_ref=src,
            dst_ref=dst,
            send_sem=self.send.at[i],
            recv_sem=self.recv.at[i],
            device_id=target,
            device_id_type=pl.DeviceIdType.MESH,
        )
        when(sends, copy.start)
        self.remote.append([copy, False, sends, receives])
        return len(self.remote) - 1

    def keep(self, src, dst):
        copy = pltpu.make_async_copy(src, dst, self.local.at[self.n_local])
        self.n_local += 1
        copy.start()
        self.locals.append(copy)

    def arrive(self, i):
        when(self.remote[i][3], self.remote[i][0].wait_recv)
        self.remote[i][1] = True

    def finish(self):
        for copy, arrived, sends, receives in self.remote:
            if not arrived:
                when(receives, copy.wait_recv)
            when(sends, copy.wait_send)
        for copy in self.locals:
            copy.wait()


def greet(axes):
    barrier = pltpu.get_barrier_semaphore()
    count = 0
    for axis in axes:
        n = lax.axis_size(axis)
        me = lax.axis_index(axis)
        for k in range(1, n):
            pl.semaphore_signal(
                barrier,
                inc=1,
                device_id={axis: lax.rem(me + k, n)},
                device_id_type=pl.DeviceIdType.MESH,
            )
            count += 1
    pl.semaphore_wait(barrier, count)


def direct(copies, kind, axis, src, dst):
    n = lax.axis_size(axis)
    me = lax.axis_index(axis)
    if kind == "next" or kind == "prev":
        copies.start(src, dst, {axis: lax.rem(me + (1 if kind == "next" else n - 1), n)})
        return
    if kind == "pair":
        copies.start(src, dst, {axis: me + 1 - 2 * lax.rem(me, 2)})
        return
    if kind == "rows":
        nz, z, c = n // 2, me // 2, lax.rem(me, 2)
        copies.keep(src.at[z], dst.at[z])
        for k in range(1, nz):
            peer = lax.rem(z + k, nz)
            copies.start(src.at[peer], dst.at[z], {axis: 2 * peer + c})
        return
    copies.keep(src.at[me] if kind == "scatter" else src, dst.at[me])
    for k in range(1, n):
        peer = lax.rem(me + k, n)
        copies.start(src.at[peer] if kind == "scatter" else src, dst.at[me], {axis: peer})


def spread_gather(copies, src, dst):
    ns, nz = lax.axis_size("sp"), lax.axis_size("dp") // 2
    s, d = lax.axis_index("sp"), lax.axis_index("dp")
    z, c = d // 2, lax.rem(d, 2)
    partner = {"dp": d + 1 - 2 * c}
    first = [
        copies.start(src.at[s], dst.at[d, s], {"dp": 2 * lax.rem(z + k, nz) + c})
        for k in range(1, nz)
    ]
    yield
    copies.keep(src, dst.at[d])
    copies.start(src, dst.at[d], partner)
    second = {}
    for k in range(1, nz):
        copies.arrive(first[k - 1])
        piece = dst.at[2 * lax.rem(z + nz - k, nz) + c, s]
        for j in range(1, ns):
            second[k, j] = copies.start(piece, piece, {"sp": lax.rem(s + j, ns)})
        copies.start(piece, piece, partner)
    yield
    for k in range(1, nz):
        for j in range(1, ns):
            copies.arrive(second[k, j])
            piece = dst.at[2 * lax.rem(z + nz - k, nz) + c, lax.rem(s + ns - j, ns)]
            copies.start(piece, piece, partner)


def line_gather(copies, src, dst):
    nz = lax.axis_size("dp") // 2
    d = lax.axis_index("dp")
    z, c = d // 2, lax.rem(d, 2)
    partner = {"dp": d + 1 - 2 * c}
    up = {"dp": 2 * lax.rem(z + 1, nz) + c}
    down = {"dp": 2 * lax.rem(z + nz - 1, nz) + c}
    below, above = {}, {}

    def send(k):
        low, high = 2 * lax.rem(z + nz - k, nz) + c, 2 * lax.rem(z + k, nz) + c
        low_src, high_src = (dst.at[low], dst.at[high]) if k else (src, src)
        below[k] = copies.start(
            low_src, dst.at[low], up, jnp.logical_and(z >= k, z < nz - 1), z >= k + 1
        )
        above[k] = copies.start(
            high_src, dst.at[high], down, jnp.logical_and(z + k < nz, z > 0), z + k + 1 < nz
        )

    send(0)
    yield
    copies.keep(src, dst.at[d])
    copies.start(src, dst.at[d], partner)
    for k in range(1, nz):
        copies.arrive(below[k - 1])
        copies.arrive(above[k - 1])
        if k < nz - 1:
            send(k)
        low, high = dst.at[2 * lax.rem(z + nz - k, nz) + c], dst.at[2 * lax.rem(z + k, nz) + c]
        copies.start(low, low, partner, z >= k, z >= k)
        copies.start(high, high, partner, z + k < nz, z + k < nz)
        yield


def run(axes, items, *refs):
    n = len(items)
    copies = Copies(*refs[2 * n :])
    greet(axes)
    waiting = []
    for i, (kind, axis) in enumerate(items):
        src, dst = refs[i], refs[n + i]
        if kind == "spread":
            waiting.append(spread_gather(copies, src, dst))
        elif kind == "line":
            waiting.append(line_gather(copies, src, dst))
        elif kind == "later":
            waiting.append(later(copies, axis, src, dst))
        else:
            direct(copies, kind, axis, src, dst)
    while waiting:
        waiting = [steps for steps in waiting if next(steps, waiting) is None]
    copies.finish()


def later(copies, axis, src, dst):
    yield
    direct(copies, "scatter", axis, src, dst)


def exchange(collective_id, *items):
    ns, nd = lax.axis_size("sp"), lax.axis_size("dp")
    shapes, remote, local = [], 0, 0
    for kind, axis, x in items:
        n = lax.axis_size(axis)
        if kind == "rows":
            shape = x.shape
            remote += n // 2 - 1
            local += 1
        elif kind in ("next", "prev", "pair"):
            shape = x.shape
            remote += 1
        elif kind in ("scatter", "later"):
            shape = x.shape
            remote += n - 1
            local += 1
        else:
            shape = (n,) + x.shape
            local += 1
            if kind == "gather":
                remote += n - 1
            elif kind == "spread":
                remote += (nd // 2 - 1) * 2 * ns + 1
            else:
                remote += (nd // 2 - 1) * 4 + 1
        shapes.append(jax.ShapeDtypeStruct(shape, x.dtype))
    axes = tuple(a for a in ("sp", "dp") if any(axis == a or kind == "spread" for kind, axis, _ in items))
    return pl.pallas_call(
        functools.partial(run, axes, tuple((kind, axis) for kind, axis, _ in items)),
        out_shape=shapes,
        in_specs=[VMEM] * len(items),
        out_specs=[VMEM] * len(items),
        scratch_shapes=[
            pltpu.SemaphoreType.DMA((remote,)),
            pltpu.SemaphoreType.DMA((remote,)),
            pltpu.SemaphoreType.DMA((max(local, 1),)),
        ],
        compiler_params=pltpu.CompilerParams(
            collective_id=collective_id, has_side_effects=True, vmem_limit_bytes=48 * 1024 * 1024
        ),
    )(*[x for _, _, x in items])


def body(value_half, gate_half, upstream, conv_taps, norm_gain, out_weight):
    f32 = jnp.float32
    tap_count = conv_taps.shape[0]
    halo = tap_count - 1
    nsp, ndp = lax.axis_size("sp"), lax.axis_size("dp")
    at_start = lax.axis_index("sp") == 0
    at_end = lax.axis_index("sp") == nsp - 1
    edge = (halo + 15) // 16 * 16

    value = value_half[0].astype(f32)
    gate = gate_half[0].astype(f32)
    length = value.shape[0]
    channels = value.shape[1]
    up = upstream[0]
    rows = out_weight.shape[0]

    tail = (value[length - edge :] * jax.nn.sigmoid(gate[length - edge :])).astype(jnp.bfloat16)
    up_blocks = jnp.swapaxes(up.reshape(length, ndp, rows), 0, 1)
    before, taps = exchange(1, ("next", "sp", tail), ("gather", "sp", conv_taps))
    before = jnp.where(at_start, 0, before)[edge - halo :]
    taps = jnp.swapaxes(taps, 0, 1).reshape(tap_count, channels)
    sig_gate = jax.nn.sigmoid(gate)
    glu = (value * sig_gate).astype(jnp.bfloat16)
    padded = jnp.concatenate([before, glu], axis=0).astype(f32)
    conv = jnp.zeros((length, padded.shape[1]), f32)
    for j in range(tap_count):
        conv = conv + taps[j] * padded[j : j + length]
    conv = conv.astype(jnp.bfloat16).astype(f32)
    mean = jnp.mean(conv, axis=-1, keepdims=True)
    centered = conv - mean
    inv = lax.rsqrt(jnp.mean(centered * centered, axis=-1, keepdims=True) + NORM_EPS)
    normed = centered * inv
    scaled = normed * norm_gain
    sig = jax.nn.sigmoid(scaled)
    activated = (scaled * sig).astype(jnp.bfloat16)

    low = channels // 4
    nz, piece = ndp // 2, rows // nsp
    core = lax.rem(lax.axis_index("dp"), 2)
    by_core = up.reshape(length, nz, 2, nsp, piece)

    def partial(which):
        columns = lax.dynamic_index_in_dim(by_core, which, 2, keepdims=False)
        columns = jnp.swapaxes(columns, 1, 2).reshape(length, nsp * nz * piece)
        return lax.dot_general(
            columns, activated[:, low:], (((0,), (0,)), ((), ())), preferred_element_type=f32
        )

    weight, act_all, up_columns, from_partner = exchange(
        2,
        ("spread", "dp", out_weight.reshape(nsp, rows // nsp, channels)),
        ("line", "dp", activated[:, :low]),
        ("later", "dp", up_blocks),
        ("pair", "dp", partial(1 - core).astype(jnp.bfloat16)),
    )
    weight = weight.reshape(ndp * rows, channels)
    act_all = act_all.reshape(ndp * length, low)
    up_columns = up_columns.reshape(ndp * length, rows)
    owned = lax.dot_general(
        up_columns, act_all, (((0,), (0,)), ((), ())), preferred_element_type=f32
    )
    summed = (partial(core) + from_partner.astype(f32)).astype(jnp.bfloat16)
    summed = summed.reshape(nsp, nz, piece, channels - low)

    grad_act = jnp.dot(up, weight, preferred_element_type=f32)
    grad_scaled = grad_act * sig * (1.0 + scaled * (1.0 - sig))
    gain_part = jnp.sum(grad_scaled * normed, axis=0)
    g = grad_scaled * norm_gain
    grad_conv = inv * (
        g
        - jnp.mean(g, axis=-1, keepdims=True)
        - normed * jnp.mean(g * normed, axis=-1, keepdims=True)
    )
    grad_conv = grad_conv.astype(jnp.bfloat16)
    after, gain_got, owned_got, summed_got = exchange(
        3,
        ("prev", "sp", grad_conv[:edge]),
        ("gather", "sp", gain_part[None]),
        ("scatter", "sp", owned.astype(jnp.bfloat16).reshape(nsp, piece, low)),
        ("scatter", "sp", summed),
    )
    after = jnp.where(at_end, 0, after)[:halo]
    extended = jnp.concatenate([grad_conv, after], axis=0).astype(f32)
    here = grad_conv.astype(f32)
    grad_glu = jnp.zeros_like(here)
    terms = []
    for j in range(tap_count):
        first = halo - j
        grad_glu = grad_glu + taps[j] * extended[first : first + length]
        terms.append(jnp.sum(here * padded[j : j + length], axis=0))
    grad_glu = grad_glu.astype(jnp.bfloat16).astype(f32)
    grad_value = (grad_glu * sig_gate).astype(jnp.bfloat16)
    grad_gate = (grad_glu * value * sig_gate * (1.0 - sig_gate)).astype(jnp.bfloat16)

    width = conv_taps.shape[1]
    tap_blocks = jnp.swapaxes(jnp.stack(terms).reshape(tap_count, nsp, width), 0, 1)
    gain_got, tap_got, low_weight, high_got = exchange(
        4,
        ("gather", "dp", jnp.sum(gain_got, axis=0)),
        ("scatter", "sp", tap_blocks),
        ("gather", "sp", jnp.sum(owned_got.astype(f32), axis=0).astype(jnp.bfloat16)),
        ("rows", "dp", jnp.sum(summed_got.astype(f32), axis=0).astype(jnp.bfloat16)),
    )
    tap_got, high_weight = exchange(
        5,
        ("gather", "dp", jnp.sum(tap_got, axis=0)),
        ("gather", "sp", jnp.sum(high_got.astype(f32), axis=0).astype(jnp.bfloat16)),
    )
    grad_gain = jnp.sum(gain_got, axis=0)[0]
    grad_taps = jnp.sum(tap_got, axis=0)
    grad_weight = jnp.concatenate(
        [low_weight.reshape(rows, low), high_weight.reshape(rows, channels - low)], axis=1
    ).astype(f32)
    return (grad_value[None], grad_gate[None], grad_taps, grad_gain, grad_weight)


def solution(mesh):
    tokens = P("dp", "sp", None)
    return jax.shard_map(
        body,
        mesh=mesh,
        in_specs=(tokens, tokens, tokens, P(None, "sp"), P(), P("dp", None)),
        out_specs=(tokens, tokens, P(None, "sp"), P(), P("dp", None)),
        check_vma=False,
    )
```

```python
import functools

import jax
import jax.numpy as jnp
from jax import lax
from jax.experimental import pallas as pl
from jax.experimental.pallas import tpu as pltpu
from jax.sharding import PartitionSpec as P

NORM_EPS = 1e-05
VMEM = pl.BlockSpec(memory_space=pltpu.VMEM)


def when(condition, act):
    if condition is None:
        act()
    else:
        pl.when(condition)(lambda: act())


class Copies:
    def __init__(self, send, recv, local):
        self.send, self.recv, self.local = send, recv, local
        self.n_remote = self.n_local = 0
        self.remote, self.locals = [], []

    def start(self, src, dst, target, sends=None, receives=None):
        i = self.n_remote
        self.n_remote += 1
        copy = pltpu.make_async_remote_copy(
            src_ref=src,
            dst_ref=dst,
            send_sem=self.send.at[i],
            recv_sem=self.recv.at[i],
            device_id=target,
            device_id_type=pl.DeviceIdType.MESH,
        )
        when(sends, copy.start)
        self.remote.append([copy, False, sends, receives])
        return len(self.remote) - 1

    def keep(self, src, dst):
        copy = pltpu.make_async_copy(src, dst, self.local.at[self.n_local])
        self.n_local += 1
        copy.start()
        self.locals.append(copy)

    def arrive(self, i):
        when(self.remote[i][3], self.remote[i][0].wait_recv)
        self.remote[i][1] = True

    def finish(self):
        for copy, arrived, sends, receives in self.remote:
            if not arrived:
                when(receives, copy.wait_recv)
            when(sends, copy.wait_send)
        for copy in self.locals:
            copy.wait()


def greet(axes):
    barrier = pltpu.get_barrier_semaphore()
    count = 0
    for axis in axes:
        n = lax.axis_size(axis)
        me = lax.axis_index(axis)
        for k in range(1, n):
            pl.semaphore_signal(
                barrier,
                inc=1,
                device_id={axis: lax.rem(me + k, n)},
                device_id_type=pl.DeviceIdType.MESH,
            )
            count += 1
    pl.semaphore_wait(barrier, count)


def direct(copies, kind, axis, src, dst):
    n = lax.axis_size(axis)
    me = lax.axis_index(axis)
    if kind == "next" or kind == "prev":
        copies.start(src, dst, {axis: lax.rem(me + (1 if kind == "next" else n - 1), n)})
        return
    if kind == "pair":
        copies.start(src, dst, {axis: me + 1 - 2 * lax.rem(me, 2)})
        return
    if kind == "rows":
        nz, z, c = n // 2, me // 2, lax.rem(me, 2)
        copies.keep(src.at[z], dst.at[z])
        for k in range(1, nz):
            peer = lax.rem(z + k, nz)
            copies.start(src.at[peer], dst.at[z], {axis: 2 * peer + c})
        return
    copies.keep(src.at[me] if kind == "scatter" else src, dst.at[me])
    for k in range(1, n):
        peer = lax.rem(me + k, n)
        copies.start(src.at[peer] if kind == "scatter" else src, dst.at[me], {axis: peer})


def spread_gather(copies, src, dst):
    ns, nz = lax.axis_size("sp"), lax.axis_size("dp") // 2
    s, d = lax.axis_index("sp"), lax.axis_index("dp")
    z, c = d // 2, lax.rem(d, 2)
    partner = {"dp": d + 1 - 2 * c}
    first = [
        copies.start(src.at[s], dst.at[d, s], {"dp": 2 * lax.rem(z + k, nz) + c})
        for k in range(1, nz)
    ]
    yield
    copies.keep(src, dst.at[d])
    copies.start(src, dst.at[d], partner)
    second = {}
    for k in range(1, nz):
        copies.arrive(first[k - 1])
        piece = dst.at[2 * lax.rem(z + nz - k, nz) + c, s]
        for j in range(1, ns):
            second[k, j] = copies.start(piece, piece, {"sp": lax.rem(s + j, ns)})
        copies.start(piece, piece, partner)
    yield
    for k in range(1, nz):
        for j in range(1, ns):
            copies.arrive(second[k, j])
            piece = dst.at[2 * lax.rem(z + nz - k, nz) + c, lax.rem(s + ns - j, ns)]
            copies.start(piece, piece, partner)


def line_gather(copies, src, dst):
    nz = lax.axis_size("dp") // 2
    d = lax.axis_index("dp")
    z, c = d // 2, lax.rem(d, 2)
    partner = {"dp": d + 1 - 2 * c}
    up = {"dp": 2 * lax.rem(z + 1, nz) + c}
    down = {"dp": 2 * lax.rem(z + nz - 1, nz) + c}
    below, above = {}, {}

    def send(k):
        low, high = 2 * lax.rem(z + nz - k, nz) + c, 2 * lax.rem(z + k, nz) + c
        low_src, high_src = (dst.at[low], dst.at[high]) if k else (src, src)
        below[k] = copies.start(
            low_src, dst.at[low], up, jnp.logical_and(z >= k, z < nz - 1), z >= k + 1
        )
        above[k] = copies.start(
            high_src, dst.at[high], down, jnp.logical_and(z + k < nz, z > 0), z + k + 1 < nz
        )

    send(0)
    yield
    copies.keep(src, dst.at[d])
    copies.start(src, dst.at[d], partner)
    for k in range(1, nz):
        copies.arrive(below[k - 1])
        copies.arrive(above[k - 1])
        if k < nz - 1:
            send(k)
        low, high = dst.at[2 * lax.rem(z + nz - k, nz) + c], dst.at[2 * lax.rem(z + k, nz) + c]
        copies.start(low, low, partner, z >= k, z >= k)
        copies.start(high, high, partner, z + k < nz, z + k < nz)
        yield


def run(axes, items, *refs):
    n = len(items)
    copies = Copies(*refs[2 * n :])
    greet(axes)
    waiting = []
    for i, (kind, axis) in enumerate(items):
        src, dst = refs[i], refs[n + i]
        if kind == "spread":
            waiting.append(spread_gather(copies, src, dst))
        elif kind == "line":
            waiting.append(line_gather(copies, src, dst))
        elif kind == "later":
            waiting.append(later(copies, axis, src, dst))
        else:
            direct(copies, kind, axis, src, dst)
    while waiting:
        waiting = [steps for steps in waiting if next(steps, waiting) is None]
    copies.finish()


def later(copies, axis, src, dst):
    yield
    direct(copies, "scatter", axis, src, dst)


def exchange(collective_id, *items):
    ns, nd = lax.axis_size("sp"), lax.axis_size("dp")
    shapes, remote, local = [], 0, 0
    for kind, axis, x in items:
        n = lax.axis_size(axis)
        if kind == "rows":
            shape = x.shape
            remote += n // 2 - 1
            local += 1
        elif kind in ("next", "prev", "pair"):
            shape = x.shape
            remote += 1
        elif kind in ("scatter", "later"):
            shape = x.shape
            remote += n - 1
            local += 1
        else:
            shape = (n,) + x.shape
            local += 1
            if kind == "gather":
                remote += n - 1
            elif kind == "spread":
                remote += (nd // 2 - 1) * 2 * ns + 1
            else:
                remote += (nd // 2 - 1) * 4 + 1
        shapes.append(jax.ShapeDtypeStruct(shape, x.dtype))
    axes = tuple(a for a in ("sp", "dp") if any(axis == a or kind == "spread" for kind, axis, _ in items))
    return pl.pallas_call(
        functools.partial(run, axes, tuple((kind, axis) for kind, axis, _ in items)),
        out_shape=shapes,
        in_specs=[VMEM] * len(items),
        out_specs=[VMEM] * len(items),
        scratch_shapes=[
            pltpu.SemaphoreType.DMA((remote,)),
            pltpu.SemaphoreType.DMA((remote,)),
            pltpu.SemaphoreType.DMA((max(local, 1),)),
        ],
        compiler_params=pltpu.CompilerParams(
            collective_id=collective_id, has_side_effects=True, vmem_limit_bytes=48 * 1024 * 1024
        ),
    )(*[x for _, _, x in items])


def body(value_half, gate_half, upstream, conv_taps, norm_gain, out_weight):
    f32 = jnp.float32
    tap_count = conv_taps.shape[0]
    halo = tap_count - 1
    nsp, ndp = lax.axis_size("sp"), lax.axis_size("dp")
    at_start = lax.axis_index("sp") == 0
    at_end = lax.axis_index("sp") == nsp - 1
    edge = (halo + 15) // 16 * 16

    value = value_half[0].astype(f32)
    gate = gate_half[0].astype(f32)
    length = value.shape[0]
    channels = value.shape[1]
    up = upstream[0]
    rows = out_weight.shape[0]

    tail = (value[length - edge :] * jax.nn.sigmoid(gate[length - edge :])).astype(jnp.bfloat16)
    up_blocks = jnp.swapaxes(up.reshape(length, ndp, rows), 0, 1)
    before, taps = exchange(1, ("next", "sp", tail), ("gather", "sp", conv_taps))
    before = jnp.where(at_start, 0, before)[edge - halo :]
    taps = jnp.swapaxes(taps, 0, 1).reshape(tap_count, channels)
    sig_gate = jax.nn.sigmoid(gate)
    glu = (value * sig_gate).astype(jnp.bfloat16)
    padded = jnp.concatenate([before, glu], axis=0).astype(f32)
    conv = jnp.zeros((length, padded.shape[1]), f32)
    for j in range(tap_count):
        conv = conv + taps[j] * padded[j : j + length]
    conv = conv.astype(jnp.bfloat16).astype(f32)
    mean = jnp.mean(conv, axis=-1, keepdims=True)
    centered = conv - mean
    inv = lax.rsqrt(jnp.mean(centered * centered, axis=-1, keepdims=True) + NORM_EPS)
    normed = centered * inv
    scaled = normed * norm_gain
    sig = jax.nn.sigmoid(scaled)
    activated = (scaled * sig).astype(jnp.bfloat16)

    low = channels * 3 // 8
    nz, piece = ndp // 2, rows // nsp
    core = lax.rem(lax.axis_index("dp"), 2)
    by_core = up.reshape(length, nz, 2, nsp, piece)

    def partial(which):
        columns = lax.dynamic_index_in_dim(by_core, which, 2, keepdims=False)
        columns = jnp.swapaxes(columns, 1, 2).reshape(length, nsp * nz * piece)
        return lax.dot_general(
            columns, activated[:, low:], (((0,), (0,)), ((), ())), preferred_element_type=f32
        )

    weight, act_all, up_columns, from_partner = exchange(
        2,
        ("spread", "dp", out_weight.reshape(nsp, rows // nsp, channels)),
        ("line", "dp", activated[:, :low]),
        ("later", "dp", up_blocks),
        ("pair", "dp", partial(1 - core).astype(jnp.bfloat16)),
    )
    weight = weight.reshape(ndp * rows, channels)
    act_all = act_all.reshape(ndp * length, low)
    up_columns = up_columns.reshape(ndp * length, rows)
    owned = lax.dot_general(
        up_columns, act_all, (((0,), (0,)), ((), ())), preferred_element_type=f32
    )
    summed = (partial(core) + from_partner.astype(f32)).astype(jnp.bfloat16)
    summed = summed.reshape(nsp, nz, piece, channels - low)

    grad_act = jnp.dot(up, weight, preferred_element_type=f32)
    grad_scaled = grad_act * sig * (1.0 + scaled * (1.0 - sig))
    gain_part = jnp.sum(grad_scaled * normed, axis=0)
    g = grad_scaled * norm_gain
    grad_conv = inv * (
        g
        - jnp.mean(g, axis=-1, keepdims=True)
        - normed * jnp.mean(g * normed, axis=-1, keepdims=True)
    )
    grad_conv = grad_conv.astype(jnp.bfloat16)
    after, gain_got, owned_got, summed_got = exchange(
        3,
        ("prev", "sp", grad_conv[:edge]),
        ("gather", "sp", gain_part[None]),
        ("scatter", "sp", owned.astype(jnp.bfloat16).reshape(nsp, piece, low)),
        ("scatter", "sp", summed),
    )
    after = jnp.where(at_end, 0, after)[:halo]
    extended = jnp.concatenate([grad_conv, after], axis=0).astype(f32)
    here = grad_conv.astype(f32)
    grad_glu = jnp.zeros_like(here)
    terms = []
    for j in range(tap_count):
        first = halo - j
        grad_glu = grad_glu + taps[j] * extended[first : first + length]
        terms.append(jnp.sum(here * padded[j : j + length], axis=0))
    grad_glu = grad_glu.astype(jnp.bfloat16).astype(f32)
    grad_value = (grad_glu * sig_gate).astype(jnp.bfloat16)
    grad_gate = (grad_glu * value * sig_gate * (1.0 - sig_gate)).astype(jnp.bfloat16)

    width = conv_taps.shape[1]
    tap_blocks = jnp.swapaxes(jnp.stack(terms).reshape(tap_count, nsp, width), 0, 1)
    gain_got, tap_got, low_weight, high_got = exchange(
        4,
        ("gather", "dp", jnp.sum(gain_got, axis=0)),
        ("scatter", "sp", tap_blocks),
        ("gather", "sp", jnp.sum(owned_got.astype(f32), axis=0).astype(jnp.bfloat16)),
        ("rows", "dp", jnp.sum(summed_got.astype(f32), axis=0).astype(jnp.bfloat16)),
    )
    tap_got, high_weight = exchange(
        5,
        ("gather", "dp", jnp.sum(tap_got, axis=0)),
        ("gather", "sp", jnp.sum(high_got.astype(f32), axis=0).astype(jnp.bfloat16)),
    )
    grad_gain = jnp.sum(gain_got, axis=0)[0]
    grad_taps = jnp.sum(tap_got, axis=0)
    grad_weight = jnp.concatenate(
        [low_weight.reshape(rows, low), high_weight.reshape(rows, channels - low)], axis=1
    ).astype(f32)
    return (grad_value[None], grad_gate[None], grad_taps, grad_gain, grad_weight)


def solution(mesh):
    tokens = P("dp", "sp", None)
    return jax.shard_map(
        body,
        mesh=mesh,
        in_specs=(tokens, tokens, tokens, P(None, "sp"), P(), P("dp", None)),
        out_specs=(tokens, tokens, P(None, "sp"), P(), P("dp", None)),
        check_vma=False,
    )
```
